32 devices in a mesh: grp: 2 (over y), dp: 2 (over x), kv: 4 (over z), tp: 2 (over core).
Axes of the slice: x: 2, y: 2, z: 4, core: 2. Of those that a mesh axis runs over, the one named last changes fastest.
Arguments:
- tokens: bfloat16 [48, 2048], P(('grp', 'dp'), 'kv'), parts along dimension 0, may hold values from -24 to 24
- norm_gain: bfloat16 [2048], P('kv'), may hold values from 0.099609375 to 1.8984375
- query_weight: bfloat16 [2048, 2048], P('kv', 'tp'), may hold values from -0.125 to 0.125
- key_weight: bfloat16 [2048, 128], replicated, may hold values from -0.125 to 0.125
- value_weight: bfloat16 [2048, 128], replicated, may hold values from -0.125 to 0.125
- gate_weight: bfloat16 [2048, 2], replicated, may hold values from -0.5 to 0.5
- output_weight: bfloat16 [2048, 2048], P('tp', 'kv'), may hold values from -1 to 1
- query_gain: bfloat16 [64], replicated, may hold values from 0.099609375 to 1.8984375
- key_gain: bfloat16 [64], replicated, may hold values from 0.099609375 to 1.8984375
- key_cache: bfloat16 [48, 2, 64, 4096], P(('grp', 'dp'), 'tp', None, 'kv'), parts along dimension 0, may hold values from -1220 to 1220
- value_cache: bfloat16 [48, 2, 64, 4096], P(('grp', 'dp'), 'tp', None, 'kv'), parts along dimension 0, may hold values from -6 to 6
- decay_cache: float32 [48, 2, 4096], P(('grp', 'dp'), 'tp', 'kv'), parts along dimension 0, may hold values from -585 to 0, as said below
- lengths: int32 [48], P(('grp', 'dp')), parts along dimension 0, may hold values from 2048 to 4096, as said below
Outputs:
- mixed: bfloat16 [48, 2048], P(('grp', 'dp'), 'kv'), parts along dimension 0
- new_key: bfloat16 [48, 2, 64], P(('grp', 'dp'), 'tp'), parts along dimension 0
- new_value: bfloat16 [48, 2, 64], P(('grp', 'dp'), 'tp'), parts along dimension 0
- new_gate: float32 [48, 2], P(('grp', 'dp'), 'tp'), parts along dimension 0
The draws below stay inside these ranges and needn't reach their ends.
There are 2 independent parts, one for each index of `grp`. The reference program is written for one: setup_inputs(seed, part) draws one part's arguments, and reference() takes and returns one part's arrays. A program takes and returns all parts, laid end to end along the dimension named above; an argument that names none is the same for every part. Nothing has to cross between parts.
Inputs may be any that keep to these rules, and one draw needn't show every extreme that they name: `decay_cache`: never positive, not falling as the position grows within a sequence, and zero at positions lengths - 1 and beyond. `lengths`: A sequence's cache holds positions 0 to its length - 1.
All inputs are finite; a program needn't handle non-finite values.
Results may differ from the reference program's by a relative error of at most 0.015.
The reference program's roundings to bfloat16 on the way count: a program that leaves them out, or rounds other values in their place, can miss the bound.
Values may be sent and summed in bfloat16 or wider, within the bound.
A program may use at most 64 MiB of HBM per device.

```python
import math
import jax
import jax.numpy as jnp
from jax import lax

D = 2048
HQ = 32
HD = 64
KEY_VALUE_HEADS = 2
POS_DEV = 1024
BATCH_ROWS = 24
CACHE_LENGTH = 4096
N_TP = 2


def sequence_lengths(key):
    return jax.random.randint(jax.random.fold_in(key, 7), (BATCH_ROWS,), CACHE_LENGTH // 2, CACHE_LENGTH + 1).astype(jnp.int32)


def draw_lengths(key, part):
    return sequence_lengths(key)


def draw_tokens(key, part):
    key_entries = jax.random.split(jax.random.fold_in(key, 3), 2)
    base = jnp.clip(jax.random.normal(key_entries[0], (BATCH_ROWS, D), jnp.float32), -5.0, 5.0)
    columns = jnp.arange(D, dtype=jnp.float32) / (D - 1)
    rough = jnp.exp(jax.random.uniform(key_entries[1], (D,), jnp.float32, math.log(0.6), math.log(1.6)))
    column_scale = jnp.exp(math.log(0.5) + math.log(3.0) * columns) * rough
    return (base * column_scale[None, :]).astype(jnp.bfloat16)


def draw_key_cache(key, part):
    key_entries = jax.random.split(jax.random.fold_in(key, 23), 1)
    base = jnp.clip(jax.random.normal(key_entries[0], (BATCH_ROWS, KEY_VALUE_HEADS, HD, CACHE_LENGTH), jnp.float32), -4.0, 4.0)
    return base.astype(jnp.bfloat16)


def draw_decay_cache(key, part):
    seq_len = sequence_lengths(key)
    key_entries = jax.random.split(jax.random.fold_in(key, 11), 7)
    fast_share = 0.5
    quick_decay = jax.random.uniform(key_entries[0], (BATCH_ROWS, KEY_VALUE_HEADS), jnp.float32) < fast_share
    fast_rate = jnp.exp(jax.random.uniform(key_entries[1], (BATCH_ROWS, KEY_VALUE_HEADS), jnp.float32, math.log(1.0 / 100.0), math.log(1.0 / 30.0)))
    slow_total = jax.random.uniform(key_entries[2], (BATCH_ROWS, KEY_VALUE_HEADS), jnp.float32, 0.4, 1.0)
    rate = jnp.where(quick_decay, fast_rate, slow_total / CACHE_LENGTH)
    block_rate = jnp.exp(jax.random.uniform(key_entries[3], (BATCH_ROWS, KEY_VALUE_HEADS, CACHE_LENGTH // POS_DEV), jnp.float32, math.log(0.5), math.log(2.0)))
    block_rate = jnp.repeat(block_rate, POS_DEV, axis=2)
    rough = jax.random.uniform(key_entries[4], (BATCH_ROWS, KEY_VALUE_HEADS, CACHE_LENGTH), jnp.float32, 0.0, 2.0)
    gate_logarithms = -rate[:, :, None] * block_rate * rough
    spike_position = jax.random.randint(key_entries[5], (BATCH_ROWS, KEY_VALUE_HEADS, 2), 0, CACHE_LENGTH)
    spike_strength = jax.random.uniform(key_entries[6], (BATCH_ROWS, KEY_VALUE_HEADS, 2), jnp.float32, math.log(0.55), math.log(0.8))
    cache_positions = jnp.arange(CACHE_LENGTH, dtype=jnp.int32)
    match_count = (cache_positions[None, None, None, :] == spike_position[:, :, :, None]).astype(jnp.float32)
    spike_events = jnp.sum(spike_strength[:, :, :, None] * match_count, axis=2)
    gate_logarithms = gate_logarithms + jnp.where(quick_decay[:, :, None], 0.0, spike_events)
    valid = cache_positions[None, None, :] < seq_len[:, None, None]
    running = jnp.cumsum(jnp.where(valid, gate_logarithms, 0.0), axis=2)
    return running[:, :, -1:] - running


def block_scale(stream_key, dims, cuts, smallest, top_value):
    factor_of = 1.0
    for position, parts in cuts:
        draws = jax.random.uniform(jax.random.fold_in(jax.random.fold_in(stream_key, 6), position), (parts,), jnp.float32, smallest / len(cuts), top_value / len(cuts))
        factor_of = factor_of * jnp.repeat(jnp.exp(draws), dims[position] // parts).reshape((-1,) + (1,) * (len(dims) - 1 - position))
    return factor_of


def normal_values(key, dims, scale, bound, pieces=(), held_as=jnp.bfloat16):
    entries = scale * jax.random.normal(key, dims, jnp.float32)
    if pieces:
        entries = entries * block_scale(key, dims, pieces, -0.22, 0.18)
    return jnp.clip(entries, -bound, bound).astype(held_as)


def setup_inputs(seed: int = 0, part: int = 0) -> dict:
    arg_keys = jax.random.split(jax.random.key(seed), 14)
    part_splits = jax.random.split(jax.random.fold_in(arg_keys[13], part), 14)
    tokens = draw_tokens(jax.random.fold_in(jax.random.fold_in(arg_keys[13], part), 71), part)
    norm_gain = jnp.clip(1.0 + 0.18 * jax.random.normal(arg_keys[1], (D,), jnp.float32), 0.099609375, 1.8984375).astype(jnp.bfloat16)
    query_weight = normal_values(arg_keys[2], (D, HQ * HD), D ** -0.5, 0.125, ((0, 4), (1, 2)))
    key_weight = normal_values(arg_keys[3], (D, KEY_VALUE_HEADS * HD), D ** -0.5, 0.125)
    value_weight = normal_values(arg_keys[4], (D, KEY_VALUE_HEADS * HD), D ** -0.5, 0.125)
    gate_weight = normal_values(arg_keys[5], (D, KEY_VALUE_HEADS), (D // 16) ** -0.5, 0.5)
    output_weight = normal_values(arg_keys[6], (HQ * HD, D), (HQ * HD // 64) ** -0.5, 1.0, ((0, 2), (1, 4)))
    query_gain = jnp.clip(1.0 + 0.18 * jax.random.normal(arg_keys[7], (HD,), jnp.float32), 0.099609375, 1.8984375).astype(jnp.bfloat16)
    key_gain = jnp.clip(1.0 + 0.18 * jax.random.normal(arg_keys[8], (HD,), jnp.float32), 0.099609375, 1.8984375).astype(jnp.bfloat16)
    key_cache = draw_key_cache(jax.random.fold_in(jax.random.fold_in(arg_keys[13], part), 71), part)
    value_cache = normal_values(part_splits[10], (BATCH_ROWS, KEY_VALUE_HEADS, HD, CACHE_LENGTH), 1.0, 6.0, ((0, 2), (1, 2), (3, 4)))
    decay_cache = draw_decay_cache(jax.random.fold_in(jax.random.fold_in(arg_keys[13], part), 71), part)
    lengths = draw_lengths(jax.random.fold_in(jax.random.fold_in(arg_keys[13], part), 71), part)
    return dict(tokens=tokens, norm_gain=norm_gain, query_weight=query_weight, key_weight=key_weight, value_weight=value_weight, gate_weight=gate_weight, output_weight=output_weight, query_gain=query_gain, key_gain=key_gain, key_cache=key_cache, value_cache=value_cache, decay_cache=decay_cache, lengths=lengths)


EPSILON = 1e-06
FLOOR = -1e+30

def head_norm(values, head_gain):
    values = values.astype(jnp.float32)
    factor = lax.rsqrt(lax.optimization_barrier(jnp.mean(values * values, axis=-1, keepdims=True)) + EPSILON)
    return (values * factor * head_gain.astype(jnp.float32)).astype(jnp.bfloat16)

def attend_one(items):
    grouped, key_entries, values, decays, length, gate, own_key, own_value = items
    group_size = HQ // KEY_VALUE_HEADS
    block_count = CACHE_LENGTH // POS_DEV
    scores = jnp.einsum('kge,kep->kgp', grouped.astype(jnp.float32), key_entries.astype(jnp.float32)) * HD ** (-0.5)
    scores = scores + decays[:, None, :] + gate[:, None, None]
    scores = scores.reshape(KEY_VALUE_HEADS, group_size, block_count, POS_DEV)
    cache_positions = jnp.arange(CACHE_LENGTH, dtype=jnp.int32).reshape(block_count, POS_DEV)
    valid = (cache_positions < length)[None, None]
    masked = jnp.where(valid, scores, FLOOR)
    block_max = lax.optimization_barrier(jnp.max(masked, axis=3))
    weights = jnp.where(valid, jnp.exp(scores - block_max[..., None]), 0.0)
    block_total = lax.optimization_barrier(jnp.sum(weights, axis=3))
    weights_low = lax.optimization_barrier(weights.astype(jnp.bfloat16)).astype(jnp.float32)
    value_blocks = values.astype(jnp.float32).reshape(KEY_VALUE_HEADS, HD, block_count, POS_DEV)
    block_values = jnp.einsum('kgjp,kejp->kgje', weights_low, value_blocks)
    own = jnp.einsum('kge,ke->kg', grouped.astype(jnp.float32), own_key.astype(jnp.float32)) * HD ** (-0.5)
    highest = jnp.maximum(lax.optimization_barrier(jnp.max(block_max, axis=2)), own)
    far_scale = jnp.exp(block_max - highest[..., None])
    own_scale = jnp.exp(own - highest)
    total = lax.optimization_barrier(jnp.sum(block_total * far_scale, axis=2)) + own_scale
    summed = lax.optimization_barrier(jnp.sum(block_values * far_scale[..., None], axis=2))
    summed = summed + own_scale[..., None] * own_value.astype(jnp.float32)[:, None, :]
    attended = (summed / total[..., None]).astype(jnp.bfloat16)
    return attended.reshape(HQ * HD)

def reference(tokens, norm_gain, query_weight, key_weight, value_weight, gate_weight, output_weight, query_gain, key_gain, key_cache, value_cache, decay_cache, lengths):
    tokens_wide = tokens.astype(jnp.float32)
    scaled = (tokens_wide * norm_gain.astype(jnp.float32)).astype(jnp.bfloat16)
    row_scale = lax.rsqrt(lax.optimization_barrier(jnp.mean(tokens_wide * tokens_wide, axis=1)) + EPSILON)
    query_raw = jnp.dot(scaled, query_weight, preferred_element_type=jnp.float32).reshape(BATCH_ROWS, HQ, HD)
    key_raw = jnp.dot(scaled, key_weight, preferred_element_type=jnp.float32).reshape(BATCH_ROWS, KEY_VALUE_HEADS, HD)
    value_raw = jnp.dot(scaled, value_weight, preferred_element_type=jnp.float32)
    gate_raw = jnp.dot(scaled, gate_weight, preferred_element_type=jnp.float32)
    queries = head_norm(query_raw, query_gain)
    new_key = head_norm(key_raw, key_gain)
    new_value = (row_scale[:, None] * value_raw).astype(jnp.bfloat16).reshape(BATCH_ROWS, KEY_VALUE_HEADS, HD)
    new_gate = jax.nn.log_sigmoid(row_scale[:, None] * gate_raw)
    grouped = queries.reshape(BATCH_ROWS, KEY_VALUE_HEADS, HQ // KEY_VALUE_HEADS, HD)
    attended = lax.map(attend_one, (grouped, key_cache, value_cache, decay_cache, lengths, new_gate, new_key, new_value))
    attended_groups = attended.reshape(BATCH_ROWS, N_TP, HQ * HD // N_TP).astype(jnp.float32)
    weight_groups = output_weight.reshape(N_TP, HQ * HD // N_TP, D).astype(jnp.float32)
    partial_value = jnp.einsum('btf,tfd->btd', attended_groups, weight_groups).astype(jnp.bfloat16)
    partial_value = lax.optimization_barrier(partial_value).astype(jnp.float32)
    mixed = lax.optimization_barrier(jnp.sum(partial_value, axis=1)).astype(jnp.bfloat16)
    return (mixed, new_key, new_value, new_gate)
```

```python
import functools

import jax
import jax.numpy as jnp
from jax import lax
from jax.experimental import pallas as pl
from jax.experimental.pallas import tpu as pltpu
from jax.sharding import PartitionSpec as P

MESH = pl.DeviceIdType.MESH
EPSILON = 1e-06
FLOOR = -1e30
SEND_DTYPE = jnp.float32
F32 = jnp.float32
BF16 = jnp.bfloat16


def kernel(
    kv_n,
    tp_n,
    lengths_ref,
    tokens_ref,
    norm_gain_ref,
    query_gain_ref,
    key_gain_ref,
    gate_hbm,
    query_hbm,
    key_w_hbm,
    value_w_hbm,
    output_hbm,
    key_hbm,
    value_hbm,
    decay_hbm,
    mixed_ref,
    new_key_ref,
    new_value_ref,
    new_gate_ref,
    query_w,
    key_w,
    value_w,
    gate_w,
    output_w,
    keys,
    values,
    decay,
    query_slots,
    small_slots,
    value_slots,
    stat_slots,
    out_slots,
    query_rows,
    att_rows,
    local_sem,
    query_send,
    query_recv,
    small_send,
    small_recv,
    value_send,
    value_recv,
    stat_send,
    stat_recv,
    out_send,
    out_recv,
):
    rows, width = tokens_ref.shape
    group = query_rows.shape[0] // rows
    head_dim, span = keys.shape[1:]
    pairs = rows // 2
    me = lax.axis_index("kv")
    tp_me = lax.axis_index("tp")
    model = width * kv_n
    chunks = value_send.shape[1]
    per_chunk = pairs // chunks

    barrier = pltpu.get_barrier_semaphore()
    for d in range(1, kv_n):
        pl.semaphore_signal(
            barrier, inc=1, device_id={"kv": lax.rem(me + d, kv_n)}, device_id_type=MESH
        )
    for d in range(1, tp_n):
        pl.semaphore_signal(
            barrier, inc=1, device_id={"tp": lax.rem(tp_me + d, tp_n)}, device_id_type=MESH
        )

    row_start = pl.multiple_of(me * width, width)
    query_chunks = query_w.shape[0]
    query_cols = query_w.shape[2]
    query_copies = [
        pltpu.make_async_copy(
            query_hbm.at[:, pl.ds(c * query_cols, query_cols)], query_w.at[c], local_sem.at[c]
        )
        for c in range(query_chunks)
    ]
    base = query_chunks
    small_copies = [
        pltpu.make_async_copy(key_w_hbm.at[pl.ds(row_start, width)], key_w, local_sem.at[base]),
        pltpu.make_async_copy(
            value_w_hbm.at[pl.ds(row_start, width)], value_w, local_sem.at[base + 1]
        ),
        pltpu.make_async_copy(
            gate_hbm.at[:, pl.ds(row_start, width)], gate_w, local_sem.at[base + 2]
        ),
    ]
    key_copy = pltpu.make_async_copy(key_hbm.at[:, 0], keys, local_sem.at[base + 3])
    decay_copy = pltpu.make_async_copy(decay_hbm, decay, local_sem.at[base + 4])
    value_copy = pltpu.make_async_copy(value_hbm.at[:, 0], values, local_sem.at[base + 5])
    output_copy = pltpu.make_async_copy(output_hbm, output_w, local_sem.at[base + 6])
    for copy in (*query_copies, *small_copies, key_copy, decay_copy, value_copy, output_copy):
        copy.start()

    def sends(slots, send_sem, recv_sem, index=None):
        out = []
        for d in range(1, kv_n):
            ref = slots.at[me] if index is None else slots.at[me, index]
            out.append(
                pltpu.make_async_remote_copy(
                    src_ref=ref,
                    dst_ref=ref,
                    send_sem=send_sem.at[d] if index is None else send_sem.at[d, index_of(index)],
                    recv_sem=recv_sem.at[me] if index is None else recv_sem.at[me, index_of(index)],
                    device_id={"kv": lax.rem(me + d, kv_n)},
                    device_id_type=MESH,
                )
            )
        return out

    def index_of(index):
        return index if isinstance(index, int) else index.start // per_chunk

    def wait_recv(slots, send_sem, recv_sem, index=None):
        for d in range(1, kv_n):
            src = lax.rem(me + d, kv_n)
            ref = slots.at[src] if index is None else slots.at[src, index]
            pltpu.make_async_remote_copy(
                src_ref=ref,
                dst_ref=ref,
                send_sem=send_sem.at[d] if index is None else send_sem.at[d, index_of(index)],
                recv_sem=recv_sem.at[src] if index is None else recv_sem.at[src, index_of(index)],
                device_id={"kv": src},
                device_id_type=MESH,
            ).wait_recv()

    tokens = tokens_ref[...].astype(F32)
    scaled = (tokens * norm_gain_ref[...].astype(F32)).astype(BF16)
    for c in range(query_chunks):
        query_copies[c].wait()
        part = jnp.dot(scaled, query_w[c], preferred_element_type=F32)
        query_slots[me, :, pl.ds(c * query_cols, query_cols)] = part.astype(query_slots.dtype)
        if c == 0:
            pass
    pl.semaphore_wait(barrier, kv_n - 1 + tp_n - 1)
    query_sends = sends(query_slots, query_send, query_recv)
    for copy in query_sends:
        copy.start()

    lane_small = lax.broadcasted_iota(jnp.int32, (rows, 128), 1)
    row_small = lax.broadcasted_iota(jnp.int32, (rows, 128), 0)
    diagonal = lane_small == row_small
    low = lane_small < head_dim

    def to_row(column):
        return jnp.sum(jnp.where(diagonal, column, 0.0), axis=0, keepdims=True)

    def to_column(row):
        return jnp.sum(jnp.where(diagonal, row, 0.0), axis=1, keepdims=True)

    for copy in small_copies:
        copy.wait()
    key_part = jnp.dot(scaled, key_w[...], preferred_element_type=F32)
    value_part = jnp.dot(scaled, value_w[...], preferred_element_type=F32)
    key_turned = pltpu.roll(key_part, head_dim, 1)
    value_turned = pltpu.roll(value_part, head_dim, 1)
    first = tp_me == 0
    key_half = jnp.where(first, key_part, key_turned)
    value_half = jnp.where(first, value_turned, value_part)
    gates = gate_w[...].astype(F32)
    gate_row = jnp.where(first, gates[0:1], gates[1:2])
    gate_part = jnp.sum(scaled.astype(F32) * gate_row, axis=1, keepdims=True)
    squares = jnp.sum(tokens * tokens, axis=1, keepdims=True)
    small_slots[me, 0:rows] = jnp.where(low, key_half, value_half)
    small_slots[me, rows : rows + 1] = to_row(gate_part)
    small_slots[me, rows + 1 : rows + 2] = to_row(squares)
    small_slots[me, rows + 2 :] = jnp.zeros((small_slots.shape[1] - rows - 2, 128), F32)
    small_sends = sends(small_slots, small_send, small_recv)
    for copy in small_sends:
        copy.start()

    wait_recv(query_slots, query_send, query_recv)
    gain = query_gain_ref[...].astype(F32)
    gain2 = jnp.concatenate([gain, gain], axis=1)

    def norm_pair(x, gain_wide):
        squared = x * x
        lo = jnp.sum(jnp.where(low, squared, 0.0), axis=1, keepdims=True)
        hi = jnp.sum(jnp.where(low, 0.0, squared), axis=1, keepdims=True)
        lo = lax.rsqrt(lo / head_dim + EPSILON)
        hi = lax.rsqrt(hi / head_dim + EPSILON)
        return (x * jnp.where(low, lo, hi) * gain_wide).astype(BF16).astype(F32)

    for c in range(group // 2):
        cols = pl.ds(c * 128, 128)
        x = query_slots[0, :, cols].astype(F32)
        for p in range(1, kv_n):
            x = x + query_slots[p, :, cols].astype(F32)
        y = norm_pair(x, gain2)
        query_rows[pl.ds(2 * c, rows, stride=group), :] = y
        query_rows[pl.ds(2 * c + 1, rows, stride=group), :] = pltpu.roll(y, head_dim, 1)

    key_copy.wait()
    decay_copy.wait()
    value_copy.wait()
    scale = head_dim ** (-0.5)
    positions = me * span + lax.broadcasted_iota(jnp.int32, (group, span), 1)
    lane = lax.broadcasted_iota(jnp.int32, (group, 128), 1)
    stat_max = jnp.full((group, 128), FLOOR, F32)
    stat_sum = jnp.zeros((group, 128), F32)

    def attend(b, stat_max, stat_sum):
        q = query_rows[group * b : group * (b + 1), 0:head_dim].astype(BF16)
        scores = jnp.dot(q, keys[b], preferred_element_type=F32) * scale + decay[b]
        valid = positions < lengths_ref[b]
        block_max = jnp.max(jnp.where(valid, scores, FLOOR), axis=1, keepdims=True)
        weights = jnp.where(valid, jnp.exp(scores - block_max), 0.0)
        block_sum = jnp.sum(weights, axis=1, keepdims=True)
        result = lax.dot_general(
            weights.astype(BF16), values[b], (((1,), (1,)), ((), ())), preferred_element_type=F32
        )
        stat_max = jnp.where(lane == b, block_max, stat_max)
        stat_sum = jnp.where(lane == b + 32, block_sum, stat_sum)
        return result, stat_max, stat_sum

    value_sends = []
    for i in range(pairs):
        one, stat_max, stat_sum = attend(i, stat_max, stat_sum)
        two, stat_max, stat_sum = attend(i + pairs, stat_max, stat_sum)
        value_slots[me, i] = jnp.concatenate([one, two], axis=1).astype(BF16)
        if (i + 1) % per_chunk == 0:
            index = pl.ds(i + 1 - per_chunk, per_chunk)
            new = sends(value_slots, value_send, value_recv, index)
            for copy in new:
                copy.start()
            value_sends += new
    half = group // 2
    packed = jnp.where(lane < 32, stat_max, stat_sum)
    stat_slots[me] = jnp.where(
        lane[:half] < 64, packed[:half], pltpu.roll(packed[half:], 64, 1)
    )
    stat_sends = sends(stat_slots, stat_send, stat_recv)
    for copy in stat_sends:
        copy.start()

    wait_recv(small_slots, small_send, small_recv)
    small = small_slots[0]
    for p in range(1, kv_n):
        small = small + small_slots[p]
    row_scale_row = lax.rsqrt(small[rows + 1 : rows + 2] / model + EPSILON)
    gate_x = row_scale_row * small[rows : rows + 1]
    gate = jnp.minimum(gate_x, 0.0) - jnp.log1p(jnp.exp(-jnp.abs(gate_x)))
    new_gate_ref[...] = to_column(gate)
    key_gain = key_gain_ref[...].astype(F32)
    both = small[:rows]
    new_key = norm_pair(both, jnp.concatenate([key_gain, key_gain], axis=1))
    new_value = (both * to_column(row_scale_row)).astype(BF16).astype(F32)
    own = jnp.zeros((group, 128), F32)
    for b in range(rows):
        new_key_ref[b] = new_key[b : b + 1, 0:head_dim].astype(BF16)
        new_value_ref[b] = new_value[b : b + 1, head_dim:].astype(BF16)
        q = query_rows[group * b : group * (b + 1), :]
        dots = jnp.sum(
            jnp.where(lane < head_dim, q * new_key[b : b + 1], 0.0), axis=1, keepdims=True
        )
        own = jnp.where(lane == b, dots * scale, own)

    wait_recv(stat_slots, stat_send, stat_recv)
    maxima, totals = [], []
    for p in range(kv_n):
        packed = stat_slots[p]
        packed = jnp.concatenate([packed, pltpu.roll(packed, 64, 1)], axis=0)
        maxima.append(packed + gate)
        totals.append(pltpu.roll(packed, 96, 1))
    real = lane < rows
    top = own
    for p in range(kv_n):
        top = jnp.maximum(top, maxima[p])
    factors = [jnp.where(real, jnp.exp(maxima[p] - top), 0.0) for p in range(kv_n)]
    own_factor = jnp.exp(own - top)
    total = own_factor
    for p in range(kv_n):
        total = total + factors[p] * totals[p]
    total = jnp.where(real, total, 1.0)
    factors = [f / total for f in factors]
    own_factor = own_factor / total

    def spread(f, i):
        return jnp.where(lane < head_dim, f[:, i : i + 1], f[:, i + pairs : i + pairs + 1])

    new_value_turned = pltpu.roll(new_value, head_dim, 1)
    for c in range(chunks):
        wait_recv(value_slots, value_send, value_recv, pl.ds(c * per_chunk, per_chunk))
        for i in range(c * per_chunk, (c + 1) * per_chunk):
            fresh = jnp.where(
                lane[0:1] < head_dim,
                new_value_turned[i : i + 1],
                new_value[i + pairs : i + pairs + 1],
            )
            acc = spread(own_factor, i) * fresh
            for p in range(kv_n):
                acc = acc + spread(factors[p], i) * value_slots[p, i].astype(F32)
            query_rows[group * i : group * (i + 1), :] = acc

    for c in range(group // 2):
        x = query_rows[pl.ds(2 * c, pairs, stride=group), :]
        y = query_rows[pl.ds(2 * c + 1, pairs, stride=group), :]
        lo = lax.broadcasted_iota(jnp.int32, (pairs, 128), 1) < head_dim
        cols = slice(c * 128, (c + 1) * 128)
        att_rows[0:pairs, cols] = jnp.where(lo, x, pltpu.roll(y, head_dim, 1))
        att_rows[pairs:rows, cols] = jnp.where(lo, pltpu.roll(x, head_dim, 1), y)

    output_copy.wait()
    partial = jnp.dot(att_rows[...].astype(BF16), output_w[...], preferred_element_type=F32)
    out_slots[tp_me] = partial.astype(BF16)
    out_sends = []
    for d in range(1, tp_n):
        copy = pltpu.make_async_remote_copy(
            src_ref=out_slots.at[tp_me],
            dst_ref=out_slots.at[tp_me],
            send_sem=out_send.at[d],
            recv_sem=out_recv.at[tp_me],
            device_id={"tp": lax.rem(tp_me + d, tp_n)},
            device_id_type=MESH,
        )
        copy.start()
        out_sends.append(copy)
    for copy in (*query_sends, *small_sends, *value_sends, *stat_sends):
        copy.wait_send()
    for d in range(1, tp_n):
        src = lax.rem(tp_me + d, tp_n)
        pltpu.make_async_remote_copy(
            src_ref=out_slots.at[src],
            dst_ref=out_slots.at[src],
            send_sem=out_send.at[d],
            recv_sem=out_recv.at[src],
            device_id={"tp": src},
            device_id_type=MESH,
        ).wait_recv()
    mixed = out_slots[0].astype(F32)
    for t in range(1, tp_n):
        mixed = mixed + out_slots[t].astype(F32)
    mixed_ref[...] = mixed.astype(BF16)
    for copy in out_sends:
        copy.wait_send()


def on_device(
    kv_n,
    tp_n,
    tokens,
    norm_gain,
    query_weight,
    key_weight,
    value_weight,
    gate_weight,
    output_weight,
    query_gain,
    key_gain,
    key_cache,
    value_cache,
    decay_cache,
    lengths,
):
    rows, width = tokens.shape
    head_dim = query_gain.shape[0]
    heads = query_weight.shape[1] // head_dim
    span = key_cache.shape[3]
    out_cols = output_weight.shape[1]
    query_chunks = 2
    chunks = 3
    pairs = rows // 2
    small_rows = -(-(rows + 2) // 8) * 8
    vmem = pl.BlockSpec(memory_space=pltpu.VMEM)
    hbm = pl.BlockSpec(memory_space=pl.ANY)
    dma = pltpu.SemaphoreType.DMA
    return pl.pallas_call(
        functools.partial(kernel, kv_n, tp_n),
        out_shape=(
            jax.ShapeDtypeStruct((rows, out_cols), BF16),
            jax.ShapeDtypeStruct((rows, 1, head_dim), BF16),
            jax.ShapeDtypeStruct((rows, 1, head_dim), BF16),
            jax.ShapeDtypeStruct((rows, 1), F32),
        ),
        in_specs=[pl.BlockSpec(memory_space=pltpu.SMEM)] + [vmem] * 4 + [hbm] * 8,
        out_specs=(vmem, vmem, vmem, vmem),
        scratch_shapes=[
            pltpu.VMEM((query_chunks, width, heads * head_dim // query_chunks), BF16),
            pltpu.VMEM((width, key_weight.shape[1]), BF16),
            pltpu.VMEM((width, value_weight.shape[1]), BF16),
            pltpu.VMEM((gate_weight.shape[1], width), BF16),
            pltpu.VMEM(output_weight.shape, BF16),
            pltpu.VMEM((rows, head_dim, span), BF16),
            pltpu.VMEM((rows, head_dim, span), BF16),
            pltpu.VMEM((rows, 1, span), F32),
            pltpu.VMEM((kv_n, rows, heads * head_dim), SEND_DTYPE),
            pltpu.VMEM((kv_n, small_rows, 128), F32),
            pltpu.VMEM((kv_n, pairs, heads, 2 * head_dim), BF16),
            pltpu.VMEM((kv_n, heads // 2, 128), F32),
            pltpu.VMEM((tp_n, rows, out_cols), BF16),
            pltpu.VMEM((rows * heads, 128), F32),
            pltpu.VMEM((rows, heads * head_dim), F32),
            dma((query_chunks + 7,)),
            dma((kv_n,)),
            dma((kv_n,)),
            dma((kv_n,)),
            dma((kv_n,)),
            dma((kv_n, chunks)),
            dma((kv_n, chunks)),
            dma((kv_n,)),
            dma((kv_n,)),
            dma((tp_n,)),
            dma((tp_n,)),
        ],
        compiler_params=pltpu.CompilerParams(
            collective_id=0, has_side_effects=True, vmem_limit_bytes=48 * 1024 * 1024
        ),
        name="decode",
    )(
        lengths,
        tokens,
        norm_gain.reshape(1, width),
        query_gain.reshape(1, head_dim),
        key_gain.reshape(1, head_dim),
        gate_weight.T,
        query_weight,
        key_weight,
        value_weight,
        output_weight,
        key_cache,
        value_cache,
        decay_cache,
    )


def solution(mesh):
    batch = P(("grp", "dp"))
    in_specs = (
        P(("grp", "dp"), "kv"),
        P("kv"),
        P("kv", "tp"),
        P(),
        P(),
        P(),
        P("tp", "kv"),
        P(),
        P(),
        P(("grp", "dp"), "tp", None, "kv"),
        P(("grp", "dp"), "tp", None, "kv"),
        P(("grp", "dp"), "tp", "kv"),
        batch,
    )
    out_specs = (
        P(("grp", "dp"), "kv"),
        P(("grp", "dp"), "tp", None),
        P(("grp", "dp"), "tp", None),
        P(("grp", "dp"), "tp"),
    )
    return jax.shard_map(
        functools.partial(on_device, mesh.shape["kv"], mesh.shape["tp"]),
        mesh=mesh,
        in_specs=in_specs,
        out_specs=out_specs,
        check_vma=False,
    )
```

```python
import functools

import jax
import jax.numpy as jnp
from jax import lax
from jax.experimental import pallas as pl
from jax.experimental.pallas import tpu as pltpu
from jax.sharding import PartitionSpec as P

MESH = pl.DeviceIdType.MESH
EPSILON = 1e-06
FLOOR = -1e30
SEND_DTYPE = jnp.float32
F32 = jnp.float32
BF16 = jnp.bfloat16


def kernel(
    kv_n,
    tp_n,
    lengths_ref,
    tokens_ref,
    norm_gain_ref,
    query_gain_ref,
    key_gain_ref,
    gate_hbm,
    query_hbm,
    key_w_hbm,
    value_w_hbm,
    output_hbm,
    key_hbm,
    value_hbm,
    decay_hbm,
    mixed_ref,
    new_key_ref,
    new_value_ref,
    new_gate_ref,
    query_w,
    key_w,
    value_w,
    gate_w,
    output_w,
    keys,
    values,
    decay,
    query_slots,
    small_slots,
    value_slots,
    stat_slots,
    out_slots,
    query_rows,
    att_rows,
    score_rows,
    weight_rows,
    local_sem,
    query_send,
    query_recv,
    small_send,
    small_recv,
    value_send,
    value_recv,
    stat_send,
    stat_recv,
    out_send,
    out_recv,
):
    rows, width = tokens_ref.shape
    group = query_rows.shape[0] // rows
    head_dim, span = keys.shape[1:]
    pairs = rows // 2
    me = lax.axis_index("kv")
    tp_me = lax.axis_index("tp")
    model = width * kv_n
    chunks = value_send.shape[1]
    per_chunk = pairs // chunks

    barrier = pltpu.get_barrier_semaphore()
    for d in range(1, kv_n):
        pl.semaphore_signal(
            barrier, inc=1, device_id={"kv": lax.rem(me + d, kv_n)}, device_id_type=MESH
        )
    for d in range(1, tp_n):
        pl.semaphore_signal(
            barrier, inc=1, device_id={"tp": lax.rem(tp_me + d, tp_n)}, device_id_type=MESH
        )

    row_start = pl.multiple_of(me * width, width)
    query_chunks = query_w.shape[0]
    query_cols = query_w.shape[2]
    query_copies = [
        pltpu.make_async_copy(
            query_hbm.at[:, pl.ds(c * query_cols, query_cols)], query_w.at[c], local_sem.at[c]
        )
        for c in range(query_chunks)
    ]
    base = query_chunks
    small_copies = [
        pltpu.make_async_copy(key_w_hbm.at[pl.ds(row_start, width)], key_w, local_sem.at[base]),
        pltpu.make_async_copy(
            value_w_hbm.at[pl.ds(row_start, width)], value_w, local_sem.at[base + 1]
        ),
        pltpu.make_async_copy(
            gate_hbm.at[:, pl.ds(row_start, width)], gate_w, local_sem.at[base + 2]
        ),
    ]
    key_copy = pltpu.make_async_copy(key_hbm.at[:, 0], keys, local_sem.at[base + 3])
    decay_copy = pltpu.make_async_copy(decay_hbm, decay, local_sem.at[base + 4])
    value_copy = pltpu.make_async_copy(value_hbm.at[:, 0], values, local_sem.at[base + 5])
    output_copy = pltpu.make_async_copy(output_hbm, output_w, local_sem.at[base + 6])
    for copy in (*query_copies, *small_copies, key_copy, decay_copy, value_copy, output_copy):
        copy.start()

    def sends(slots, send_sem, recv_sem, index=None):
        out = []
        for d in range(1, kv_n):
            ref = slots.at[me] if index is None else slots.at[me, index]
            out.append(
                pltpu.make_async_remote_copy(
                    src_ref=ref,
                    dst_ref=ref,
                    send_sem=send_sem.at[d] if index is None else send_sem.at[d, index_of(index)],
                    recv_sem=recv_sem.at[me] if index is None else recv_sem.at[me, index_of(index)],
                    device_id={"kv": lax.rem(me + d, kv_n)},
                    device_id_type=MESH,
                )
            )
        return out

    def index_of(index):
        return index if isinstance(index, int) else index.start // per_chunk

    def wait_recv(slots, send_sem, recv_sem, index=None):
        for d in range(1, kv_n):
            src = lax.rem(me + d, kv_n)
            ref = slots.at[src] if index is None else slots.at[src, index]
            pltpu.make_async_remote_copy(
                src_ref=ref,
                dst_ref=ref,
                send_sem=send_sem.at[d] if index is None else send_sem.at[d, index_of(index)],
                recv_sem=recv_sem.at[src] if index is None else recv_sem.at[src, index_of(index)],
                device_id={"kv": src},
                device_id_type=MESH,
            ).wait_recv()

    tokens = tokens_ref[...].astype(F32)
    scaled = (tokens * norm_gain_ref[...].astype(F32).reshape(1, width)).astype(BF16)
    for c in range(query_chunks):
        query_copies[c].wait()
        part = jnp.dot(scaled, query_w[c], preferred_element_type=F32)
        query_slots[me, :, pl.ds(c * query_cols, query_cols)] = part.astype(query_slots.dtype)
        if c == 0:
            pass
    pl.semaphore_wait(barrier, kv_n - 1 + tp_n - 1)
    query_sends = sends(query_slots, query_send, query_recv)
    for copy in query_sends:
        copy.start()

    lane_small = lax.broadcasted_iota(jnp.int32, (rows, 128), 1)
    row_small = lax.broadcasted_iota(jnp.int32, (rows, 128), 0)
    diagonal = lane_small == row_small
    low = lane_small < head_dim

    def to_row(column):
        return jnp.sum(jnp.where(diagonal, column, 0.0), axis=0, keepdims=True)

    def to_column(row):
        return jnp.sum(jnp.where(diagonal, row, 0.0), axis=1, keepdims=True)

    for copy in small_copies:
        copy.wait()
    key_part = jnp.dot(scaled, key_w[...], preferred_element_type=F32)
    value_part = jnp.dot(scaled, value_w[...], preferred_element_type=F32)
    key_turned = pltpu.roll(key_part, head_dim, 1)
    value_turned = pltpu.roll(value_part, head_dim, 1)
    first = tp_me == 0
    key_half = jnp.where(first, key_part, key_turned)
    value_half = jnp.where(first, value_turned, value_part)
    gates = gate_w[...].astype(F32)
    gate_row = jnp.where(first, gates[0:1], gates[1:2])
    gate_part = jnp.sum(scaled.astype(F32) * gate_row, axis=1, keepdims=True)
    squares = jnp.sum(tokens * tokens, axis=1, keepdims=True)
    small_slots[me, 0:rows] = jnp.where(low, key_half, value_half)
    small_slots[me, rows : rows + 1] = to_row(gate_part)
    small_slots[me, rows + 1 : rows + 2] = to_row(squares)
    small_slots[me, rows + 2 :] = jnp.zeros((small_slots.shape[1] - rows - 2, 128), F32)
    small_sends = sends(small_slots, small_send, small_recv)
    for copy in small_sends:
        copy.start()

    scale = head_dim ** (-0.5)
    decay_copy.wait()
    positions = me * span + lax.broadcasted_iota(jnp.int32, (1, span), 1)
    for b in range(rows):
        decay[b] = jnp.where(positions < lengths_ref[b], decay[b], FLOOR)
    key_copy.wait()
    value_copy.wait()

    wait_recv(query_slots, query_send, query_recv)
    gain = query_gain_ref[...].astype(F32).reshape(1, head_dim)
    gain2 = jnp.concatenate([gain, gain], axis=1)

    def norm_pair(x, gain_wide):
        squared = x * x
        lo = jnp.sum(jnp.where(low, squared, 0.0), axis=1, keepdims=True)
        hi = jnp.sum(jnp.where(low, 0.0, squared), axis=1, keepdims=True)
        lo = lax.rsqrt(lo / head_dim + EPSILON)
        hi = lax.rsqrt(hi / head_dim + EPSILON)
        return (x * jnp.where(low, lo, hi) * gain_wide).astype(BF16).astype(F32)

    for c in range(group // 2):
        cols = pl.ds(c * 128, 128)
        x = query_slots[0, :, cols].astype(F32)
        for p in range(1, kv_n):
            x = x + query_slots[p, :, cols].astype(F32)
        y = norm_pair(x, gain2) * scale
        query_rows[pl.ds(2 * c, rows, stride=group), :] = y
        query_rows[pl.ds(2 * c + 1, rows, stride=group), :] = pltpu.roll(y, head_dim, 1)

    lane = lax.broadcasted_iota(jnp.int32, (group, 128), 1)
    stat_max = jnp.full((group, 128), FLOOR, F32)
    stat_sum = jnp.zeros((group, 128), F32)

    def rows_of(b):
        return slice(group * b, group * (b + 1))

    value_sends = []
    for chunk in range(chunks):
        first_pair = chunk * per_chunk
        members = []
        for i in range(first_pair, first_pair + per_chunk):
            members += [i, i + pairs]
        maxes = {}
        for b in members:
            q = query_rows[rows_of(b), 0:head_dim].astype(BF16)
            scores = jnp.dot(q, keys[b], preferred_element_type=F32) + decay[b]
            score_rows[rows_of(b), :] = scores
            maxes[b] = jnp.max(scores, axis=1, keepdims=True)
            stat_max = jnp.where(lane == b, maxes[b], stat_max)
        for b in members:
            weights = jnp.exp(score_rows[rows_of(b), :] - maxes[b])
            weight_rows[rows_of(b), :] = weights.astype(BF16)
            block_sum = jnp.sum(weights, axis=1, keepdims=True)
            stat_sum = jnp.where(lane == b + 32, block_sum, stat_sum)
        results = {}
        for b in members:
            results[b] = lax.dot_general(
                weight_rows[rows_of(b), :],
                values[b],
                (((1,), (1,)), ((), ())),
                preferred_element_type=F32,
            )
        for i in range(first_pair, first_pair + per_chunk):
            value_slots[me, i] = jnp.concatenate(
                [results[i], results[i + pairs]], axis=1
            ).astype(BF16)
        new = sends(value_slots, value_send, value_recv, pl.ds(first_pair, per_chunk))
        for copy in new:
            copy.start()
        value_sends += new
    half = group // 2
    packed = jnp.where(lane < 32, stat_max, stat_sum)
    stat_slots[me] = jnp.where(
        lane[:half] < 64, packed[:half], pltpu.roll(packed[half:], 64, 1)
    )
    stat_sends = sends(stat_slots, stat_send, stat_recv)
    for copy in stat_sends:
        copy.start()

    wait_recv(small_slots, small_send, small_recv)
    small = small_slots[0]
    for p in range(1, kv_n):
        small = small + small_slots[p]
    row_scale_row = lax.rsqrt(small[rows + 1 : rows + 2] / model + EPSILON)
    gate_x = row_scale_row * small[rows : rows + 1]
    gate = jnp.minimum(gate_x, 0.0) - jnp.log1p(jnp.exp(-jnp.abs(gate_x)))
    new_gate_ref[...] = gate[:, 0:rows]
    key_gain = key_gain_ref[...].astype(F32).reshape(1, head_dim)
    both = small[:rows]
    new_key = norm_pair(both, jnp.concatenate([key_gain, key_gain], axis=1))
    new_value = (both * to_column(row_scale_row)).astype(BF16).astype(F32)
    new_value_turned = pltpu.roll(new_value, head_dim, 1)
    new_key_ref[...] = new_key[:, 0:head_dim].astype(BF16)
    new_value_ref[...] = new_value_turned[:, 0:head_dim].astype(BF16)
    own = jnp.zeros((group, 128), F32)
    for b in range(rows):
        q = query_rows[group * b : group * (b + 1), :]
        dots = jnp.sum(
            jnp.where(lane < head_dim, q * new_key[b : b + 1], 0.0), axis=1, keepdims=True
        )
        own = jnp.where(lane == b, dots, own)

    wait_recv(stat_slots, stat_send, stat_recv)
    maxima, totals = [], []
    for p in range(kv_n):
        packed = stat_slots[p]
        packed = jnp.concatenate([packed, pltpu.roll(packed, 64, 1)], axis=0)
        maxima.append(packed + gate)
        totals.append(pltpu.roll(packed, 96, 1))
    real = lane < rows
    top = own
    for p in range(kv_n):
        top = jnp.maximum(top, maxima[p])
    factors = [jnp.where(real, jnp.exp(maxima[p] - top), 0.0) for p in range(kv_n)]
    own_factor = jnp.exp(own - top)
    total = own_factor
    for p in range(kv_n):
        total = total + factors[p] * totals[p]
    total = jnp.where(real, total, 1.0)
    factors = [f / total for f in factors]
    own_factor = own_factor / total

    def spread(f, i):
        return jnp.where(lane < head_dim, f[:, i : i + 1], f[:, i + pairs : i + pairs + 1])

    for c in range(chunks):
        wait_recv(value_slots, value_send, value_recv, pl.ds(c * per_chunk, per_chunk))
        for i in range(c * per_chunk, (c + 1) * per_chunk):
            fresh = jnp.where(
                lane[0:1] < head_dim,
                new_value_turned[i : i + 1],
                new_value[i + pairs : i + pairs + 1],
            )
            acc = spread(own_factor, i) * fresh
            for p in range(kv_n):
                acc = acc + spread(factors[p], i) * value_slots[p, i].astype(F32)
            query_rows[group * i : group * (i + 1), :] = acc

    for c in range(group // 2):
        x = query_rows[pl.ds(2 * c, pairs, stride=group), :]
        y = query_rows[pl.ds(2 * c + 1, pairs, stride=group), :]
        lo = lax.broadcasted_iota(jnp.int32, (pairs, 128), 1) < head_dim
        cols = slice(c * 128, (c + 1) * 128)
        att_rows[0:pairs, cols] = jnp.where(lo, x, pltpu.roll(y, head_dim, 1))
        att_rows[pairs:rows, cols] = jnp.where(lo, pltpu.roll(x, head_dim, 1), y)

    output_copy.wait()
    partial = jnp.dot(att_rows[...].astype(BF16), output_w[...], preferred_element_type=F32)
    out_slots[tp_me] = partial.astype(BF16)
    out_sends = []
    for d in range(1, tp_n):
        copy = pltpu.make_async_remote_copy(
            src_ref=out_slots.at[tp_me],
            dst_ref=out_slots.at[tp_me],
            send_sem=out_send.at[d],
            recv_sem=out_recv.at[tp_me],
            device_id={"tp": lax.rem(tp_me + d, tp_n)},
            device_id_type=MESH,
        )
        copy.start()
        out_sends.append(copy)
    for copy in (*query_sends, *small_sends, *value_sends, *stat_sends):
        copy.wait_send()
    for d in range(1, tp_n):
        src = lax.rem(tp_me + d, tp_n)
        pltpu.make_async_remote_copy(
            src_ref=out_slots.at[src],
            dst_ref=out_slots.at[src],
            send_sem=out_send.at[d],
            recv_sem=out_recv.at[src],
            device_id={"tp": src},
            device_id_type=MESH,
        ).wait_recv()
    mixed = out_slots[0].astype(F32)
    for t in range(1, tp_n):
        mixed = mixed + out_slots[t].astype(F32)
    mixed_ref[...] = mixed.astype(BF16)
    for copy in out_sends:
        copy.wait_send()


def emit(*refs):
    half = len(refs) // 2
    for source, target in zip(refs[:half], refs[half:]):
        target[...] = source[...]


def on_device(
    kv_n,
    tp_n,
    tokens,
    norm_gain,
    query_weight,
    key_weight,
    value_weight,
    gate_weight,
    output_weight,
    query_gain,
    key_gain,
    key_cache,
    value_cache,
    decay_cache,
    lengths,
):
    rows, width = tokens.shape
    head_dim = query_gain.shape[0]
    heads = query_weight.shape[1] // head_dim
    span = key_cache.shape[3]
    out_cols = output_weight.shape[1]
    query_chunks = 2
    chunks = 3
    pairs = rows // 2
    small_rows = -(-(rows + 2) // 8) * 8
    vmem = pl.BlockSpec(memory_space=pltpu.VMEM)
    hbm = pl.BlockSpec(memory_space=pltpu.HBM)
    dma = pltpu.SemaphoreType.DMA
    results = pl.pallas_call(
        functools.partial(kernel, kv_n, tp_n),
        out_shape=(
            jax.ShapeDtypeStruct((rows, out_cols), BF16),
            jax.ShapeDtypeStruct((rows, head_dim), BF16),
            jax.ShapeDtypeStruct((rows, head_dim), BF16),
            jax.ShapeDtypeStruct((1, rows), F32),
        ),
        in_specs=[pl.BlockSpec(memory_space=pltpu.SMEM)] + [vmem] * 4 + [hbm] * 8,
        out_specs=(vmem, vmem, vmem, vmem),
        scratch_shapes=[
            pltpu.VMEM((query_chunks, width, heads * head_dim // query_chunks), BF16),
            pltpu.VMEM((width, key_weight.shape[1]), BF16),
            pltpu.VMEM((width, value_weight.shape[1]), BF16),
            pltpu.VMEM((gate_weight.shape[1], width), BF16),
            pltpu.VMEM(output_weight.shape, BF16),
            pltpu.VMEM((rows, head_dim, span), BF16),
            pltpu.VMEM((rows, head_dim, span), BF16),
            pltpu.VMEM((rows, 1, span), F32),
            pltpu.VMEM((kv_n, rows, heads * head_dim), SEND_DTYPE),
            pltpu.VMEM((kv_n, small_rows, 128), F32),
            pltpu.VMEM((kv_n, pairs, heads, 2 * head_dim), BF16),
            pltpu.VMEM((kv_n, heads // 2, 128), F32),
            pltpu.VMEM((tp_n, rows, out_cols), BF16),
            pltpu.VMEM((rows * heads, 128), F32),
            pltpu.VMEM((rows, heads * head_dim), F32),
            pltpu.VMEM((rows * heads, span), F32),
            pltpu.VMEM((rows * heads, span), BF16),
            dma((query_chunks + 7,)),
            dma((kv_n,)),
            dma((kv_n,)),
            dma((kv_n,)),
            dma((kv_n,)),
            dma((kv_n, chunks)),
            dma((kv_n, chunks)),
            dma((kv_n,)),
            dma((kv_n,)),
            dma((tp_n,)),
            dma((tp_n,)),
        ],
        compiler_params=pltpu.CompilerParams(
            collective_id=0, has_side_effects=True, vmem_limit_bytes=67043328
        ),
        name="decode",
    )(
        lengths,
        tokens,
        norm_gain,
        query_gain,
        key_gain,
        gate_weight.T,
        query_weight,
        key_weight,
        value_weight,
        output_weight,
        key_cache,
        value_cache,
        decay_cache,
    )
    mixed, new_key, new_value, new_gate = pl.pallas_call(
        emit,
        out_shape=tuple(jax.ShapeDtypeStruct(r.shape, r.dtype) for r in results),
        in_specs=[vmem] * 4,
        out_specs=(vmem,) * 4,
        compiler_params=pltpu.CompilerParams(vmem_limit_bytes=67043328),
        name="emit",
    )(*results)
    return (
        mixed,
        new_key.reshape(rows, 1, head_dim),
        new_value.reshape(rows, 1, head_dim),
        new_gate.T,
    )


def solution(mesh):
    batch = P(("grp", "dp"))
    in_specs = (
        P(("grp", "dp"), "kv"),
        P("kv"),
        P("kv", "tp"),
        P(),
        P(),
        P(),
        P("tp", "kv"),
        P(),
        P(),
        P(("grp", "dp"), "tp", None, "kv"),
        P(("grp", "dp"), "tp", None, "kv"),
        P(("grp", "dp"), "tp", "kv"),
        batch,
    )
    out_specs = (
        P(("grp", "dp"), "kv"),
        P(("grp", "dp"), "tp", None),
        P(("grp", "dp"), "tp", None),
        P(("grp", "dp"), "tp"),
    )
    return jax.shard_map(
        functools.partial(on_device, mesh.shape["kv"], mesh.shape["tp"]),
        mesh=mesh,
        in_specs=in_specs,
        out_specs=out_specs,
        check_vma=False,
    )
```
